32 devices in a mesh: ep: 8 (over z, x), tp: 4 (over y, core).
Axes of the slice: x: 2, y: 2, z: 4, core: 2. Of those that a mesh axis runs over, the one named last changes fastest.
Arguments:
- residual: bfloat16 [512, 4096], P('ep', 'tp'), may hold values from -64 to 64
- routes: int32 [512, 2], P('ep'), may hold values from 0 to 7, all different within a row; in each aligned block of 64 rows (0 to 63, 64 to 127, ...) at most 32 rows name the same one
- route_weights: float32 [512, 2], P('ep'), may hold values from 0.2 to 1
- state_prev: float32 [512, 2, 64, 64], P('ep', None, 'tp'), may hold values from -6 to 6
- mix_gain: float32 [4096], replicated, may hold values from 0.1 to 1.9
- ffn_gain: float32 [4096], replicated, may hold values from 0.1 to 1.9
- w_in: bfloat16 [4096, 1024], P(None, 'tp'), may hold values from -0.09375 to 0.09375
- decay_rate: float32 [64, 64], P('tp'), may hold values from 0.5 to 8
- rotation: float32 [64, 64], P('tp'), may hold values from 0 to 200
- log_step: float32 [64], P('tp'), may hold values from -3.9 to -1.2
- in_re: float32 [64, 64, 16], P('tp'), may hold values from -1 to 1
- in_im: float32 [64, 64, 16], P('tp'), may hold values from -1 to 1
- read_re: float32 [64, 16, 64], P('tp'), may hold values from -0.5 to 0.5
- read_im: float32 [64, 16, 64], P('tp'), may hold values from -0.5 to 0.5
- skip_gain: float32 [64, 16], P('tp'), may hold values from -4 to 4
- w_glu: bfloat16 [1024, 1024], P(None, 'tp'), may hold values from -0.1875 to 0.1875
- w_out: bfloat16 [1024, 4096], P('tp'), may hold values from -0.1875 to 0.1875
- w_gate: bfloat16 [8, 4096, 5632], P('ep', None, 'tp'), may hold values from -0.09375 to 0.09375
- w_up: bfloat16 [8, 4096, 5632], P('ep', None, 'tp'), may hold values from -0.09375 to 0.09375
- w_down: bfloat16 [8, 5632, 4096], P('ep', 'tp'), may hold values from -0.078125 to 0.078125
Outputs:
- layer_out: bfloat16 [512, 4096], P('ep', 'tp')
- state_next: float32 [512, 2, 64, 64], P('ep', None, 'tp')
The draws below stay inside these ranges and needn't reach their ends.
Inputs may be any that keep to these rules, and one draw needn't show every extreme that they name: `routes`: each row names 2 different experts. In each aligned block of 64 rows (the rows of one index of ep) no expert is named more than 32 times, a bound that some block reaches.
All inputs are finite; a program needn't handle non-finite values.
Results may differ from the reference program's by a relative error of at most 0.012.
Values may be sent and summed in bfloat16 or wider, within the bound.
A program may use at most 128 MiB of HBM per device.

```python
import math
import jax
import jax.numpy as jnp
import numpy as np
from jax import lax

D = 4096
CHAN = 1024
GROUP_CH = 16
GROUPS = 64
STATE = 64
FF_EXP = 5632
TOPK = 2
SEQ_GRP = 64
SEQS = 512
EXPERTS = 8
CAP = 32
N_EP = 8
N_TP = 4


def draw_residual(key, part):
    first_key, second_key = jax.random.split(jax.random.fold_in(key, 11))
    column_pos = jnp.arange(D, dtype=jnp.float32) / D
    row_scale = jnp.exp(math.log(10.0) * (jax.random.uniform(second_key, (SEQS, 1), jnp.float32) - 0.5))
    base_values = jnp.clip(jax.random.normal(first_key, (SEQS, D), jnp.float32), -6.0, 6.0)
    column_scale = jnp.exp(math.log(10.0) * (column_pos - 0.5))
    return (base_values * column_scale[None, :] * row_scale).astype(jnp.bfloat16)


def shard_levels(rng, dims, cuts, low, largest):
    def one(dim, shards_of):
        heights = jax.random.uniform(jax.random.fold_in(jax.random.fold_in(rng, 6), dim), (shards_of,), jnp.float32, low / len(cuts), largest / len(cuts))
        return jnp.repeat(jnp.exp(heights), dims[dim] // shards_of).reshape((-1,) + (1,) * (len(dims) - dim - 1))

    factor_of = one(*cuts[0])
    for cut in cuts[1:]:
        factor_of = factor_of * one(*cut)
    return factor_of


def deal_out(own_key, own, number, rows, number_of, top, limit, lean):
    sequence = jax.random.permutation(own_key, number_of)
    packed, usual = portions_of(number_of, rows * top, limit, lean, True), portions_of(number_of, rows * top, limit, lean, False)
    places = jnp.arange(number_of)

    def named(sizes, turn):
        used = int((sizes > 0).sum())
        fixed = max(1, used // 4)
        moved = fixed + (places - fixed + turn * (used - fixed)) % max(1, number_of - fixed)
        return jnp.zeros((number_of,), jnp.int32).at[sequence[jnp.where(places < fixed, places, moved)]].set(jnp.asarray(sizes, jnp.int32))

    sizes = jnp.where(number % 4 == 0, named(packed, number // 4), named(usual, number - number // 4 - 1))
    mixed = jax.random.permutation(jax.random.fold_in(own, 3), number_of)
    giver, taker = mixed[0:number_of // 2 * 2:2], mixed[1:number_of // 2 * 2:2]
    room = jnp.minimum(sizes[giver] - 1, limit - sizes[taker]) // 2
    room = jnp.where((giver == sequence[0]) | (taker == sequence[0]) | (sizes[taker] == 0), 0, jnp.maximum(room, 0))
    moved = jax.random.randint(jax.random.fold_in(own, 4), (number_of // 2,), 0, 1 << 20) % (room + 1)
    sizes = sizes.at[giver].add(-moved).at[taker].add(moved)
    items = jnp.searchsorted(jnp.cumsum(sizes), jnp.arange(rows * top), side="right").astype(jnp.int32)
    listing = items.reshape(top, rows).T
    listing = listing[jax.random.permutation(jax.random.fold_in(own, 1), rows)]
    turn = jax.random.randint(jax.random.fold_in(own, 2), (rows, 1), 0, top)
    return jnp.take_along_axis(listing, (jnp.arange(top)[None, :] + turn) % top, axis=1)


def portions_of(amount, total, reach, lean, full):
    portions = [(1 << 20) // math.isqrt(rank ** lean) + 1 for rank in range(1, amount + 1)]
    largest = reach if full else min(reach, max(-(-total // amount), total * portions[0] // sum(portions)))
    least = 1 if total - largest >= amount - 1 else 0
    holding, surplus = [largest] + [least] * (amount - 1), total - largest - least * (amount - 1)
    while surplus > 0:
        movable = [i for i in range(1, amount) if holding[i] < largest] or [i for i in range(1, amount) if holding[i] < reach]
        mass, left = sum([portions[i] for i in movable]), surplus
        for i in movable:
            addition = min(reach - holding[i], max(1, left * portions[i] // mass), surplus)
            holding[i] = holding[i] + addition
            surplus = surplus - addition
    return np.array(holding)


def noise(rng, dims, deviation, bound, shards=(), held_as=jnp.bfloat16):
    factor_of = shard_levels(rng, dims, shards, -0.22, 0.18) if shards else 1.0
    array = jax.random.normal(rng, dims, jnp.float32) * deviation * factor_of
    return jnp.minimum(jnp.maximum(array, -bound), bound).astype(held_as)


def setup_inputs(seed: int = 0) -> dict:
    keys = jax.random.split(jax.random.key(seed), 21)
    residual = draw_residual(jax.random.fold_in(keys[20], 71), 0)
    routes_keys = jax.random.split(jax.random.fold_in(keys[1], 1), SEQS // SEQ_GRP)
    routes_turns = jax.random.permutation(jax.random.fold_in(keys[1], 3), SEQS // SEQ_GRP)
    routes = jax.vmap(lambda own, number: deal_out(jax.random.fold_in(keys[1], 2), own, number, SEQ_GRP, EXPERTS, TOPK, CAP, 1))(routes_keys, routes_turns).reshape((SEQS, TOPK))
    route_weights = jnp.clip(0.2 + 0.8 * jax.random.uniform(keys[2], (SEQS, TOPK), jnp.float32) ** shard_levels(keys[2], (SEQS, TOPK), ((0, 8),), -0.2, 0.2), 0.2, 1.0)
    state_prev = noise(keys[3], (SEQS, 2, GROUPS, STATE), 1.0, 6.0, ((0, 8), (2, 4)), jnp.float32)
    mix_gain = jnp.clip(1.0 + 0.18 * jax.random.normal(keys[4], (D,), jnp.float32), 0.1, 1.9)
    ffn_gain = jnp.clip(1.0 + 0.18 * jax.random.normal(keys[5], (D,), jnp.float32), 0.1, 1.9)
    w_in = noise(keys[6], (D, CHAN), D ** -0.5, 0.09375, ((1, 4),))
    decay_rate = jnp.clip(jnp.exp(math.log(8.0) - 2.7725887 * jax.random.uniform(keys[7], (GROUPS, STATE), jnp.float32) ** shard_levels(keys[7], (GROUPS, STATE), ((0, 4),), -0.2, 0.2)), 0.5, 8.0)
    rotation = jnp.clip(200.0 * jax.random.uniform(keys[8], (GROUPS, STATE), jnp.float32) ** shard_levels(keys[8], (GROUPS, STATE), ((0, 4),), -0.2, 0.2), 0.0, 200.0)
    log_step = jnp.clip(-3.9 + 2.7 * jax.random.uniform(keys[9], (GROUPS,), jnp.float32) ** shard_levels(keys[9], (GROUPS,), ((0, 4),), -0.2, 0.2), -3.9, -1.2)
    in_re = noise(keys[10], (GROUPS, STATE, GROUP_CH), (2 * GROUP_CH) ** -0.5, 1.0, ((0, 4),), jnp.float32)
    in_im = noise(keys[11], (GROUPS, STATE, GROUP_CH), (2 * GROUP_CH) ** -0.5, 1.0, ((0, 4),), jnp.float32)
    read_re = noise(keys[12], (GROUPS, GROUP_CH, STATE), (2 * STATE) ** -0.5, 0.5, ((0, 4),), jnp.float32)
    read_im = noise(keys[13], (GROUPS, GROUP_CH, STATE), (2 * STATE) ** -0.5, 0.5, ((0, 4),), jnp.float32)
    skip_gain = noise(keys[14], (GROUPS, GROUP_CH), 1.0, 4.0, ((0, 4),), jnp.float32)
    w_glu = noise(keys[15], (CHAN, CHAN), CHAN ** -0.5, 0.1875, ((1, 4),))
    w_out = noise(keys[16], (CHAN, D), CHAN ** -0.5, 0.1875, ((0, 4),))
    w_gate = noise(keys[17], (EXPERTS, D, FF_EXP), D ** -0.5, 0.09375, ((0, 8), (2, 4)))
    w_up = noise(keys[18], (EXPERTS, D, FF_EXP), D ** -0.5, 0.09375, ((0, 8), (2, 4)))
    w_down = noise(keys[19], (EXPERTS, FF_EXP, D), FF_EXP ** -0.5, 0.078125, ((0, 8), (1, 4)))
    return dict(residual=residual, routes=routes, route_weights=route_weights, state_prev=state_prev, mix_gain=mix_gain, ffn_gain=ffn_gain, w_in=w_in, decay_rate=decay_rate, rotation=rotation, log_step=log_step, in_re=in_re, in_im=in_im, read_re=read_re, read_im=read_im, skip_gain=skip_gain, w_glu=w_glu, w_out=w_out, w_gate=w_gate, w_up=w_up, w_down=w_down)


epsilon = 1e-06
highest = lax.Precision.HIGHEST

def inverse_rms(values):
    return lax.rsqrt(lax.optimization_barrier(jnp.mean(values * values, axis=-1, keepdims=True)) + epsilon)

def state_mixer(u_in, state_prev, decay_rate, rotation, log_step, in_re, in_im, read_re, read_im, skip_gain):
    batch_rows = u_in.shape[0]
    groups = decay_rate.shape[0]
    grouped = u_in.astype(jnp.float32).reshape(batch_rows, groups, GROUP_CH)
    step_size = jnp.exp(log_step)[:, None]
    real_part = -decay_rate
    magnitude = jnp.exp(real_part * step_size)
    decay_re = magnitude * jnp.cos(rotation * step_size)
    decay_im = magnitude * jnp.sin(rotation * step_size)
    denominator = real_part * real_part + rotation * rotation
    lift_re = ((decay_re - 1.0) * real_part + decay_im * rotation) / denominator
    lift_im = (decay_im * real_part - (decay_re - 1.0) * rotation) / denominator
    map_re = lift_re[..., None] * in_re - lift_im[..., None] * in_im
    map_im = lift_re[..., None] * in_im + lift_im[..., None] * in_re
    drive_re = jnp.einsum('gph,bgh->bgp', map_re, grouped, precision=highest)
    drive_im = jnp.einsum('gph,bgh->bgp', map_im, grouped, precision=highest)
    old_re = state_prev[:, 0]
    old_im = state_prev[:, 1]
    new_re = decay_re * old_re - decay_im * old_im + drive_re
    new_im = decay_re * old_im + decay_im * old_re + drive_im
    output = jnp.einsum('ghp,bgp->bgh', read_re, new_re, precision=highest) - jnp.einsum('ghp,bgp->bgh', read_im, new_im, precision=highest) + skip_gain * grouped
    return (jax.nn.gelu(output.reshape(batch_rows, -1)), jnp.stack([new_re, new_im], axis=1))

def reference(residual, routes, route_weights, state_prev, mix_gain, ffn_gain, w_in, decay_rate, rotation, log_step, in_re, in_im, read_re, read_im, skip_gain, w_glu, w_out, w_gate, w_up, w_down):
    source = residual.astype(jnp.float32)
    normed_mix = (source * inverse_rms(source) * mix_gain).astype(jnp.bfloat16)
    u_in = jnp.dot(normed_mix, w_in, preferred_element_type=jnp.float32).astype(jnp.bfloat16)
    mixer_act, state_next = state_mixer(u_in, state_prev, decay_rate, rotation, log_step, in_re, in_im, read_re, read_im, skip_gain)
    mixer_bf = mixer_act.astype(jnp.bfloat16)
    glu_logit = jnp.dot(mixer_bf, w_glu, preferred_element_type=jnp.float32)
    mixed = (mixer_act * jax.nn.sigmoid(glu_logit)).astype(jnp.bfloat16)
    block_width = CHAN // N_TP
    branch = jnp.zeros((SEQS, D), jnp.float32)
    for shard in range(N_TP):
        partial_block = jnp.dot(mixed[:, shard * block_width:(shard + 1) * block_width], w_out[shard * block_width:(shard + 1) * block_width], preferred_element_type=jnp.float32).astype(jnp.bfloat16)
        branch = branch + lax.optimization_barrier(partial_block).astype(jnp.float32)
    after_mix = (source + branch).astype(jnp.bfloat16)
    after_float = after_mix.astype(jnp.float32)
    normed_ffn = (after_float * inverse_rms(after_float) * ffn_gain).astype(jnp.bfloat16)
    expert_ids = jnp.arange(EXPERTS, dtype=jnp.int32)
    onehot = (routes[:, :, None] == expert_ids).astype(jnp.int32)
    blocked = onehot.reshape(N_EP, SEQ_GRP * TOPK, EXPERTS)
    before = jnp.cumsum(blocked, axis=1) - blocked
    slot_index = lax.optimization_barrier(jnp.sum(before * blocked, axis=-1)).reshape(SEQS, TOPK)
    group_of_row = jnp.arange(SEQS, dtype=jnp.int32) // SEQ_GRP
    position = group_of_row[:, None] * CAP + slot_index
    columns = jnp.arange(N_EP * CAP, dtype=jnp.int32)
    hidden_width = FF_EXP // N_TP
    normed_float = normed_ffn.astype(jnp.float32)

    def apply_expert(running, expert):
        matches = (routes == expert)[:, :, None] & (position[:, :, None] == columns)
        select = jnp.any(matches, axis=1).astype(jnp.float32)
        weighting = lax.optimization_barrier(jnp.sum(jnp.where(matches, route_weights[:, :, None], 0.0), axis=1))
        expert_in = jnp.dot(select.T, normed_float, precision=highest).astype(jnp.bfloat16)
        gate_value = jnp.dot(expert_in, w_gate[expert], preferred_element_type=jnp.float32)
        up_value = jnp.dot(expert_in, w_up[expert], preferred_element_type=jnp.float32)
        hidden = (jax.nn.silu(gate_value) * up_value).astype(jnp.bfloat16)
        down_weight = w_down[expert]
        summed = jnp.zeros((N_EP * CAP, D), jnp.float32)
        for shard in range(N_TP):
            partial_block = jnp.dot(hidden[:, shard * hidden_width:(shard + 1) * hidden_width], down_weight[shard * hidden_width:(shard + 1) * hidden_width], preferred_element_type=jnp.float32).astype(jnp.bfloat16)
            summed = summed + lax.optimization_barrier(partial_block).astype(jnp.float32)
        expert_out = summed.astype(jnp.bfloat16)
        added = jnp.dot(weighting, expert_out.astype(jnp.float32), precision=highest)
        return (running + added, None)
    combined, _ = lax.scan(apply_expert, jnp.zeros((SEQS, D), jnp.float32), expert_ids)
    layer_out = (after_float + combined).astype(jnp.bfloat16)
    return (layer_out, state_next)
```

```python
import functools

import jax
import jax.numpy as jnp
from jax import lax
from jax.experimental import pallas as pl
from jax.experimental.pallas import tpu as pltpu
from jax.sharding import PartitionSpec as P

GROUP_CH = 16
TOPK = 2


epsilon = 1e-06
highest = lax.Precision.HIGHEST


def state_mixer(
    u_in, state_prev, decay_rate, rotation, log_step, in_re, in_im, read_re, read_im, skip_gain
):
    batch_rows = u_in.shape[0]
    groups = decay_rate.shape[0]
    grouped = u_in.astype(jnp.float32).reshape(batch_rows, groups, GROUP_CH)
    step_size = jnp.exp(log_step)[:, None]
    real_part = -decay_rate
    magnitude = jnp.exp(real_part * step_size)
    decay_re = magnitude * jnp.cos(rotation * step_size)
    decay_im = magnitude * jnp.sin(rotation * step_size)
    denominator = real_part * real_part + rotation * rotation
    lift_re = ((decay_re - 1.0) * real_part + decay_im * rotation) / denominator
    lift_im = (decay_im * real_part - (decay_re - 1.0) * rotation) / denominator
    map_re = lift_re[..., None] * in_re - lift_im[..., None] * in_im
    map_im = lift_re[..., None] * in_im + lift_im[..., None] * in_re
    drive_re = jnp.einsum("gph,bgh->bgp", map_re, grouped, precision=highest)
    drive_im = jnp.einsum("gph,bgh->bgp", map_im, grouped, precision=highest)
    old_re = state_prev[:, 0]
    old_im = state_prev[:, 1]
    new_re = decay_re * old_re - decay_im * old_im + drive_re
    new_im = decay_re * old_im + decay_im * old_re + drive_im
    output = (
        jnp.einsum("ghp,bgp->bgh", read_re, new_re, precision=highest)
        - jnp.einsum("ghp,bgp->bgh", read_im, new_im, precision=highest)
        + skip_gain * grouped
    )
    return (jax.nn.gelu(output.reshape(batch_rows, -1)), jnp.stack([new_re, new_im], axis=1))


MESH = pl.DeviceIdType.MESH


def remote(src, dst, send_sem, recv_sem, target):
    return pltpu.make_async_remote_copy(
        src_ref=src,
        dst_ref=dst,
        send_sem=send_sem,
        recv_sem=recv_sem,
        device_id=target,
        device_id_type=MESH,
    )


def enter(targets):
    barrier = pltpu.get_barrier_semaphore()
    for target in targets:
        pl.semaphore_signal(barrier, inc=1, device_id=target, device_id_type=MESH)
    pl.semaphore_wait(barrier, len(targets))


def columns(place, width):
    return pl.ds(pl.multiple_of(place * width, width), width)


def branch_kernel(
    chips,
    part_ref,
    resid_ref,
    gain_ref,
    after_ref,
    normed_ref,
    near,
    staged,
    far,
    squares,
    near_send,
    near_recv,
    far_send,
    far_recv,
    sq_send,
    sq_recv,
):
    ep, tp = lax.axis_index("ep"), lax.axis_index("tp")
    core, chip = lax.rem(tp, 2), lax.div(tp, 2)
    width = resid_ref.shape[1]
    members = 2 * chips
    others = [lax.rem(chip + k, chips) for k in range(1, chips)]
    peers = [lax.rem(tp + k, members) for k in range(1, members)]
    partner = (ep, 2 * chip + 1 - core)
    enter([(ep, p) for p in peers])
    order = others + [chip]
    first = []
    for i, y in enumerate(order):
        copy = remote(
            part_ref.at[:, columns(2 * y + 1 - core, width)],
            near.at[i],
            near_send.at[i],
            near_recv.at[i],
            partner,
        )
        copy.start()
        first.append(copy)
    second = []
    for i, y in enumerate(others):
        first[i].wait_recv()
        own = part_ref[:, columns(2 * y + core, width)].astype(jnp.float32)
        staged[i] = (own + near[i].astype(jnp.float32)).astype(jnp.bfloat16)
        copy = remote(staged.at[i], far.at[i], far_send.at[i], far_recv.at[i], (ep, 2 * y + core))
        copy.start()
        second.append(copy)
    first[-1].wait_recv()
    total = part_ref[:, columns(tp, width)].astype(jnp.float32)
    total = total + near[chips - 1].astype(jnp.float32)
    for i in range(chips - 1):
        second[i].wait_recv()
        total = total + far[i].astype(jnp.float32)
    after = (resid_ref[...].astype(jnp.float32) + total).astype(jnp.bfloat16)
    after_ref[...] = after
    after = after.astype(jnp.float32)
    own_sum = jnp.sum(after * after, axis=1, keepdims=True)
    squares[0] = jnp.broadcast_to(own_sum, squares.shape[1:])
    third = []
    for k, p in enumerate(peers):
        copy = remote(
            squares.at[0], squares.at[k + 1], sq_send.at[k], sq_recv.at[k], (ep, p)
        )
        copy.start()
        third.append(copy)
    row_sum = squares[0]
    for k in range(members - 1):
        third[k].wait_recv()
        row_sum = row_sum + squares[k + 1]
    scale = lax.rsqrt(row_sum[:, :1] / (width * members) + epsilon)
    normed_ref[...] = (after * scale * gain_ref[...]).astype(jnp.bfloat16)
    for copy in first + second + third:
        copy.wait_send()


def dispatch_kernel(
    chips,
    out_ref_in,
    rows_ref,
    ep_send,
    ep_recv,
    pair_send,
    pair_recv,
    far_send,
    far_recv,
    relay_send,
    relay_recv,
):
    ep, tp = lax.axis_index("ep"), lax.axis_index("tp")
    experts, _, width = out_ref_in.shape
    core, chip = lax.rem(tp, 2), lax.div(tp, 2)
    others = [lax.rem(chip + k, chips) for k in range(1, chips)]
    away = [lax.rem(ep + k, experts) for k in range(1, experts)]
    partner = (ep, 2 * chip + 1 - core)
    enter([(e, tp) for e in away] + [partner] + [(ep, 2 * y + core) for y in others])
    mine = columns(tp, width)
    sends = []
    for k, e in enumerate(away):
        copy = remote(
            out_ref_in.at[e], rows_ref.at[ep, :, mine], ep_send.at[k], ep_recv.at[k], (e, tp)
        )
        copy.start()
        sends.append(copy)
    rows_ref[ep, :, mine] = out_ref_in[ep]
    for k in range(experts):
        source = lax.rem(ep + experts - k, experts)
        if k == 0:
            block = out_ref_in.at[ep]
        else:
            block = rows_ref.at[source, :, mine]
            remote(block, block, ep_send.at[k - 1], ep_recv.at[k - 1], partner).wait_recv()
        landing = rows_ref.at[source, :, mine]
        for j, y in enumerate(others):
            copy = remote(
                block, landing, far_send.at[k, j], far_recv.at[k, j], (ep, 2 * y + core)
            )
            copy.start()
            sends.append(copy)
        copy = remote(block, landing, pair_send.at[k], pair_recv.at[k], partner)
        copy.start()
        sends.append(copy)
    for k in range(experts):
        source = lax.rem(ep + experts - k, experts)
        for j in range(chips - 1):
            y = lax.rem(chip + chips - 1 - j, chips)
            block = rows_ref.at[source, :, columns(2 * y + core, width)]
            remote(block, block, far_send.at[k, j], far_recv.at[k, j], partner).wait_recv()
            copy = remote(block, block, relay_send.at[k, j], relay_recv.at[k, j], partner)
            copy.start()
            sends.append(copy)
    for k in range(experts):
        source = lax.rem(ep + experts - k, experts)
        block = rows_ref.at[source, :, columns(2 * chip + 1 - core, width)]
        remote(block, block, pair_send.at[k], pair_recv.at[k], partner).wait_recv()
        for j in range(chips - 1):
            y = lax.rem(chip + chips - 1 - j, chips)
            block = rows_ref.at[source, :, columns(2 * y + 1 - core, width)]
            remote(block, block, relay_send.at[k, j], relay_recv.at[k, j], partner).wait_recv()
    for copy in sends:
        copy.wait_send()


def return_kernel(
    chips,
    part_ref,
    back_ref,
    near,
    staged,
    far,
    summed,
    near_send,
    near_recv,
    far_send,
    far_recv,
    ep_send,
    ep_recv,
):
    ep, tp = lax.axis_index("ep"), lax.axis_index("tp")
    experts, _, width = back_ref.shape
    core, chip = lax.rem(tp, 2), lax.div(tp, 2)
    others = [lax.rem(chip + k, chips) for k in range(1, chips)]
    away = [lax.rem(ep + k, experts) for k in range(1, experts)]
    targets = away + [ep]
    partner = (ep, 2 * chip + 1 - core)
    enter([(e, tp) for e in away] + [partner] + [(ep, 2 * y + core) for y in others])
    order = others + [chip]
    sends = []
    for k, e in enumerate(targets):
        for i, y in enumerate(order):
            copy = remote(
                part_ref.at[e, :, columns(2 * y + 1 - core, width)],
                near.at[k, i],
                near_send.at[k, i],
                near_recv.at[k, i],
                partner,
            )
            copy.start()
            sends.append(copy)
    for k, e in enumerate(targets):
        for i, y in enumerate(others):
            landed = near.at[k, i]
            remote(landed, landed, near_send.at[k, i], near_recv.at[k, i], partner).wait_recv()
            own = part_ref[e, :, columns(2 * y + core, width)].astype(jnp.float32)
            staged[k, i] = (own + near[k, i].astype(jnp.float32)).astype(jnp.bfloat16)
            copy = remote(
                staged.at[k, i],
                far.at[k, i],
                far_send.at[k, i],
                far_recv.at[k, i],
                (ep, 2 * y + core),
            )
            copy.start()
            sends.append(copy)
    for k, e in enumerate(targets):
        last = chips - 1
        landed = near.at[k, last]
        remote(landed, landed, near_send.at[k, last], near_recv.at[k, last], partner).wait_recv()
        total = part_ref[e, :, columns(tp, width)].astype(jnp.float32)
        total = total + near[k, last].astype(jnp.float32)
        for i in range(last):
            landed = far.at[k, i]
            remote(landed, landed, far_send.at[k, i], far_recv.at[k, i], partner).wait_recv()
            total = total + far[k, i].astype(jnp.float32)
        if k == experts - 1:
            back_ref[ep] = total.astype(jnp.bfloat16)
        else:
            summed[k] = total.astype(jnp.bfloat16)
            copy = remote(
                summed.at[k], back_ref.at[ep], ep_send.at[k], ep_recv.at[k], (e, tp)
            )
            copy.start()
            sends.append(copy)
    for k in range(1, experts):
        landed = back_ref.at[lax.rem(ep + experts - k, experts)]
        remote(landed, landed, ep_send.at[k - 1], ep_recv.at[k - 1], partner).wait_recv()
    for copy in sends:
        copy.wait_send()


def call(kernel, out_shape, scratch, ident, name, *operands):
    vmem = pl.BlockSpec(memory_space=pltpu.VMEM)
    return pl.pallas_call(
        kernel,
        out_shape=out_shape,
        in_specs=[vmem] * len(operands),
        out_specs=jax.tree.map(lambda _: vmem, out_shape),
        scratch_shapes=scratch,
        compiler_params=pltpu.CompilerParams(collective_id=ident, has_side_effects=True),
        name=name,
    )(*operands)


def sum_branch(partial_out, residual, gain, chips):
    rows, width = residual.shape
    dma = pltpu.SemaphoreType.DMA
    shape = jax.ShapeDtypeStruct(residual.shape, jnp.bfloat16)
    hops, peers = chips - 1, 2 * chips - 1
    scratch = [
        pltpu.VMEM((chips, rows, width), jnp.bfloat16),
        pltpu.VMEM((hops, rows, width), jnp.bfloat16),
        pltpu.VMEM((hops, rows, width), jnp.bfloat16),
        pltpu.VMEM((2 * chips, rows, 128), jnp.float32),
        dma((chips,)),
        dma((chips,)),
        dma((hops,)),
        dma((hops,)),
        dma((peers,)),
        dma((peers,)),
    ]
    body = functools.partial(branch_kernel, chips)
    return call(body, (shape, shape), scratch, 0, "sum_branch", partial_out, residual, gain)


def dispatch_rows(outbound, chips):
    experts, capacity, width = outbound.shape
    dma = pltpu.SemaphoreType.DMA
    hops = chips - 1
    shape = jax.ShapeDtypeStruct((experts, capacity, width * 2 * chips), jnp.bfloat16)
    scratch = [dma((experts - 1,))] * 2 + [dma((experts,))] * 2 + [dma((experts, hops))] * 4
    body = functools.partial(dispatch_kernel, chips)
    return call(body, shape, scratch, 1, "dispatch_rows", outbound)


def return_rows(partial_sum, chips):
    experts, capacity, full = partial_sum.shape
    width, hops = full // (2 * chips), chips - 1
    dma = pltpu.SemaphoreType.DMA
    shape = jax.ShapeDtypeStruct((experts, capacity, width), jnp.bfloat16)
    scratch = [
        pltpu.VMEM((experts, chips, capacity, width), jnp.bfloat16),
        pltpu.VMEM((experts, hops, capacity, width), jnp.bfloat16),
        pltpu.VMEM((experts, hops, capacity, width), jnp.bfloat16),
        pltpu.VMEM((experts - 1, capacity, width), jnp.bfloat16),
        dma((experts, chips)),
        dma((experts, chips)),
        dma((experts, hops)),
        dma((experts, hops)),
        dma((experts - 1,)),
        dma((experts - 1,)),
    ]
    body = functools.partial(return_kernel, chips)
    return call(body, shape, scratch, 2, "return_rows", partial_sum)


def per_device(
    residual,
    routes,
    route_weights,
    state_prev,
    mix_gain,
    ffn_gain,
    w_in,
    decay_rate,
    rotation,
    log_step,
    in_re,
    in_im,
    read_re,
    read_im,
    skip_gain,
    w_glu,
    w_out,
    w_gate,
    w_up,
    w_down,
):
    shard_width = residual.shape[1]
    full_width = shard_width * lax.axis_size("tp")
    tp_place = lax.axis_index("tp")
    experts_all = lax.axis_size("ep")
    seq_rows = residual.shape[0]
    capacity = 2 * seq_rows * TOPK // experts_all
    chips = lax.axis_size("tp") // 2
    whole_rows = lax.all_gather(residual, "tp", axis=1, tiled=True).astype(jnp.float32)
    squares = jnp.sum(whole_rows * whole_rows, axis=1)
    scale_rows = lax.rsqrt(squares / full_width + epsilon)[:, None]
    gathered = (whole_rows * scale_rows * mix_gain).astype(jnp.bfloat16)
    u_in = jnp.dot(gathered, w_in, preferred_element_type=jnp.float32).astype(jnp.bfloat16)
    mixer_act, state_next = state_mixer(
        u_in, state_prev, decay_rate, rotation, log_step, in_re, in_im, read_re, read_im, skip_gain
    )
    mixer_bf = mixer_act.astype(jnp.bfloat16)
    all_channels = lax.all_gather(mixer_bf, "tp", axis=1, tiled=True)
    glu_logit = jnp.dot(all_channels, w_glu, preferred_element_type=jnp.float32)
    mixed = (mixer_act * jax.nn.sigmoid(glu_logit)).astype(jnp.bfloat16)
    partial_out = jnp.dot(mixed, w_out, preferred_element_type=jnp.float32)
    ffn_own = lax.dynamic_slice_in_dim(ffn_gain, tp_place * shard_width, shard_width)
    after_mix, normed_ffn = sum_branch(
        partial_out.astype(jnp.bfloat16), residual, ffn_own[None, :], chips
    )
    flat_routes = routes.reshape(-1)
    onehot = (flat_routes[:, None] == jnp.arange(experts_all, dtype=jnp.int32)).astype(jnp.int32)
    before = jnp.cumsum(onehot, axis=0) - onehot
    slot_index = jnp.sum(before * onehot, axis=1)
    destination = (flat_routes * capacity + slot_index).reshape(seq_rows, TOPK)
    matches = destination[:, :, None] == jnp.arange(experts_all * capacity, dtype=jnp.int32)
    dispatch_map = jnp.sum(matches.astype(jnp.float32), axis=1).astype(jnp.bfloat16)
    combine_map = jnp.sum(jnp.where(matches, route_weights[:, :, None], 0.0), axis=1)
    outbound = jnp.einsum("bj,bd->jd", dispatch_map, normed_ffn, preferred_element_type=jnp.float32)
    outbound = outbound.astype(jnp.bfloat16).reshape(experts_all, capacity, shard_width)
    arrived = dispatch_rows(outbound, chips)
    sources, slots_here, row_width = arrived.shape
    flat_rows = arrived.reshape(sources * slots_here, row_width)
    gate_value = jnp.dot(flat_rows, w_gate[0], preferred_element_type=jnp.float32)
    up_value = jnp.dot(flat_rows, w_up[0], preferred_element_type=jnp.float32)
    hidden = (jax.nn.silu(gate_value) * up_value).astype(jnp.bfloat16)
    partial_sum = jnp.dot(hidden, w_down[0], preferred_element_type=jnp.float32)
    partial_sum = partial_sum.reshape(sources, slots_here, row_width)
    came_back = return_rows(partial_sum.astype(jnp.bfloat16), chips)
    came_back = came_back.reshape(experts_all * capacity, shard_width).astype(jnp.float32)
    combined = jnp.dot(combine_map, came_back, precision=highest)
    layer_out = (after_mix.astype(jnp.float32) + combined).astype(jnp.bfloat16)
    return (layer_out, state_next)


def solution(mesh):
    return jax.shard_map(
        per_device,
        mesh=mesh,
        in_specs=(
            P("ep", "tp"),
            P("ep", None),
            P("ep", None),
            P("ep", None, "tp", None),
            P(),
            P(),
            P(None, "tp"),
            P("tp", None),
            P("tp", None),
            P("tp"),
            P("tp", None, None),
            P("tp", None, None),
            P("tp", None, None),
            P("tp", None, None),
            P("tp", None),
            P(None, "tp"),
            P("tp", None),
            P("ep", None, "tp"),
            P("ep", None, "tp"),
            P("ep", "tp", None),
        ),
        out_specs=(P("ep", "tp"), P("ep", None, "tp", None)),
        check_vma=False,
    )
```
